32 devices in a mesh: sp: 8 (over z, x), tp: 4 (over y, core).
Axes of the slice: x: 2, y: 2, z: 4, core: 2. Of those that a mesh axis runs over, the one named last changes fastest.
Arguments:
- upstream: bfloat16 [2048, 2048], P('sp'), may hold values from -6 to 6
- stream: bfloat16 [2048, 2048], P('sp'), may hold values from -10 to 10
- routes: int32 [2048, 2], P('sp'), may hold values from 0 to 7, all different within a row; in each aligned block of 256 rows (0 to 255, 256 to 511, ...) at most 128 rows name the same one
- route_weights: float32 [2048, 2], P('sp'), may hold values from 0.1 to 1
- glu_value: bfloat16 [2048, 512], P('sp', 'tp'), may hold values from -6 to 6
- glu_gate: bfloat16 [2048, 512], P('sp', 'tp'), may hold values from -10 to 10
- conv_taps: float32 [31, 512], P(None, 'tp'), may hold values from -1 to 1
- conv_saved: bfloat16 [2048, 512], P('sp', 'tp'), may hold values from -600 to 600
- out_proj: bfloat16 [2048, 512], P(None, 'tp'), may hold values from -0.25 to 0.25
- expert_gate: bfloat16 [8, 2048, 2048], P('sp', None, 'tp'), may hold values from -0.125 to 0.125
- expert_up: bfloat16 [8, 2048, 2048], P('sp', None, 'tp'), may hold values from -0.125 to 0.125
- expert_down: bfloat16 [8, 2048, 2048], P('sp', 'tp'), may hold values from -0.125 to 0.125
Outputs:
- grad_stream: bfloat16 [2048, 2048], P('sp', 'tp')
- grad_value: bfloat16 [2048, 512], P('sp', 'tp')
- grad_gate: bfloat16 [2048, 512], P('sp', 'tp')
- grad_out_proj: float32 [2048, 512], P('sp', 'tp')
- grad_expert_gate: float32 [8, 2048, 2048], P('sp', None, 'tp')
- grad_expert_up: float32 [8, 2048, 2048], P('sp', None, 'tp')
- grad_expert_down: float32 [8, 2048, 2048], P('sp', 'tp')
The draws below stay inside these ranges and needn't reach their ends.
Inputs may be any that keep to these rules, and one draw needn't show every extreme that they name: `routes`: each row names 2 different experts; among the 256 rows of one index of sp no expert is named more than 128 times, a bound that some block reaches.
All inputs are finite; a program needn't handle non-finite values.
Results may differ from the reference program's by a relative error of at most 0.014.
Values may be sent and summed in bfloat16 or wider, within the bound.
A program may use at most 128 MiB of HBM per device.

```python
import math
from functools import partial
import jax
import jax.numpy as jnp
import numpy as np
from jax import lax

D = 2048
FF = 2048
CW = 512
KW = 31
TOPK = 2
TOK_DEV = 256
TOKENS = 2048
EXPERTS = 8
CAP = 128
N_SP = 8
N_TP = 4


def draw_conv_saved(key, part):
    key_values, key_rows = jax.random.split(key, 2)
    column_scale = 10.0 ** (jnp.arange(CW, dtype=jnp.float32) / CW)
    values = jnp.clip(jax.random.normal(key_values, (TOKENS, CW), jnp.float32), -4.0, 4.0)
    row_scale = jnp.exp(jax.random.uniform(key_rows, (TOKENS, 1), jnp.float32, 0.0, math.log(10.0)))
    result = values * column_scale[None, :] * row_scale
    return result.astype(jnp.bfloat16)


def raised(drawn, key, source, target, shards_of, factor):
    def block_of(axis_at):
        return (jnp.arange(drawn.shape[axis_at]) // (drawn.shape[axis_at] // shards_of)).reshape((-1,) + (1,) * (drawn.ndim - 1 - axis_at))

    first = jax.random.permutation(key, shards_of)[block_of(target)]
    other_side = (block_of(target) + shards_of // 2) % shards_of
    return jnp.where((block_of(source) == first) | (block_of(source) == other_side), factor * drawn, drawn)


def block_scale(stream_key, shape, pieces, least, largest):
    factor_of, own = 1.0, jax.random.fold_in(stream_key, 6)
    for dim, parts in pieces:
        heights = jnp.exp(jax.random.uniform(jax.random.fold_in(own, dim), (parts,), jnp.float32, least / len(pieces), largest / len(pieces)))
        factor_of = factor_of * jnp.repeat(heights, shape[dim] // parts).reshape([-1 if axis == dim else 1 for axis in range(len(shape))])
    return factor_of


def routed_block(stream_key, own, number, rows, count, top, reach, skew):
    order = jax.random.permutation(stream_key, count)
    packed, usual = load_shares(count, rows * top, reach, skew, True), load_shares(count, rows * top, reach, skew, False)
    places = jnp.arange(count)

    def named(sizes, offset_by):
        used = int((sizes > 0).sum())
        fixed = max(1, used // 4)
        moved = fixed + (places - fixed + offset_by * (used - fixed)) % max(1, count - fixed)
        return jnp.zeros((count,), jnp.int32).at[order[jnp.where(places < fixed, places, moved)]].set(jnp.asarray(sizes, jnp.int32))

    sizes = jnp.where(number % 4 == 0, named(packed, number // 4), named(usual, number - number // 4 - 1))
    mixed = jax.random.permutation(jax.random.fold_in(own, 3), count)
    source_of, receiver = mixed[0:count // 2 * 2:2], mixed[1:count // 2 * 2:2]
    slack = jnp.minimum(sizes[source_of] - 1, reach - sizes[receiver]) // 2
    slack = jnp.where((source_of == order[0]) | (receiver == order[0]) | (sizes[receiver] == 0), 0, jnp.maximum(slack, 0))
    moved = jax.random.randint(jax.random.fold_in(own, 4), (count // 2,), 0, 1 << 20) % (slack + 1)
    sizes = sizes.at[source_of].add(-moved).at[receiver].add(moved)
    items = jnp.searchsorted(jnp.cumsum(sizes), jnp.arange(rows * top), side="right").astype(jnp.int32)
    table = items.reshape(top, rows).T
    table = table[jax.random.permutation(jax.random.fold_in(own, 1), rows)]
    offset_by = jax.random.randint(jax.random.fold_in(own, 2), (rows, 1), 0, top)
    return jnp.take_along_axis(table, (jnp.arange(top)[None, :] + offset_by) % top, axis=1)


def load_shares(amount, total, most, lean, full):
    loads = [(1 << 20) // math.isqrt(standing ** lean) + 1 for standing in range(1, amount + 1)]
    largest = most if full else min(most, max(-(-total // amount), total * loads[0] // sum(loads)))
    least = 1 if total - largest >= amount - 1 else 0
    given, surplus = [largest] + [least] * (amount - 1), total - largest - least * (amount - 1)
    while surplus > 0:
        free = [i for i in range(1, amount) if given[i] < largest] or [i for i in range(1, amount) if given[i] < most]
        mass, left = sum([loads[i] for i in free]), surplus
        for i in free:
            more = min(most - given[i], max(1, left * loads[i] // mass), surplus)
            given[i] = given[i] + more
            surplus = surplus - more
    return np.array(given)


def bell_draw(rng, extent, deviation, limit, cuts=(), kind=jnp.bfloat16):
    entries = jax.random.normal(rng, extent, jnp.float32) * deviation
    if len(cuts) > 0:
        entries = block_scale(rng, extent, cuts, -0.22, 0.18) * entries
    return jnp.clip(entries, min=-limit, max=limit).astype(kind)


def heavy_noise(stream_key, shape, scale, most, cuts, heavy, kind=jnp.bfloat16):
    array = scale * jax.random.normal(stream_key, shape, jnp.float32)
    if cuts:
        array = array * block_scale(stream_key, shape, cuts, -0.22, 0.18)
    return jnp.clip(raised(array, jax.random.fold_in(stream_key, 3), *heavy), -most, most).astype(kind)


def setup_inputs(seed: int = 0) -> dict:
    seeds = jax.random.split(jax.random.key(seed), 13)
    upstream = heavy_noise(seeds[0], (TOKENS, D), 1.0, 6.0, ((0, 8),), (0, 1, 8, 2.0))
    stream = bell_draw(seeds[1], (TOKENS, D), 1.0, 10.0, ((0, 8),))
    routes_keys = jax.random.split(jax.random.fold_in(seeds[2], 1), TOKENS // TOK_DEV)
    routes_turns = jax.random.permutation(jax.random.fold_in(seeds[2], 3), TOKENS // TOK_DEV)
    routes = jax.vmap(lambda own, number: routed_block(jax.random.fold_in(seeds[2], 2), own, number, TOK_DEV, EXPERTS, TOPK, CAP, 2))(routes_keys, routes_turns).reshape((TOKENS, TOPK))
    route_weights = jnp.clip(0.1 + 0.9 * jax.random.uniform(seeds[3], (TOKENS, TOPK), jnp.float32) ** block_scale(seeds[3], (TOKENS, TOPK), ((0, 8),), -0.2, 0.2), 0.1, 1.0)
    glu_value = bell_draw(seeds[4], (TOKENS, CW), 1.0, 6.0, ((0, 8), (1, 4)))
    glu_gate = bell_draw(seeds[5], (TOKENS, CW), 2.0, 10.0, ((0, 8), (1, 4)))
    conv_taps = bell_draw(seeds[6], (KW, CW), KW ** -0.5, 1.0, ((1, 4),), jnp.float32)
    conv_saved = draw_conv_saved(jax.random.fold_in(seeds[12], 71), 0)
    out_proj = bell_draw(seeds[8], (D, CW), CW ** -0.5, 0.25, ((1, 4),))
    expert_gate = bell_draw(seeds[9], (EXPERTS, D, FF), D ** -0.5, 0.125, ((0, 8), (2, 4)))
    expert_up = bell_draw(seeds[10], (EXPERTS, D, FF), D ** -0.5, 0.125, ((0, 8), (2, 4)))
    expert_down = bell_draw(seeds[11], (EXPERTS, FF, D), FF ** -0.5, 0.125, ((0, 8), (1, 4)))
    return {"upstream": upstream, "stream": stream, "routes": routes, "route_weights": route_weights, "glu_value": glu_value, "glu_gate": glu_gate, "conv_taps": conv_taps, "conv_saved": conv_saved, "out_proj": out_proj, "expert_gate": expert_gate, "expert_up": expert_up, "expert_down": expert_down}


clamp_limit = 7.0
glu_alpha = 1.702
norm_eps = 1e-05

def contract_rows(left, right):
    return lax.dot_general(left, right, (((0,), (0,)), ((), ())), preferred_element_type=jnp.float32)

def times_transposed(left, right):
    return lax.dot_general(left, right, (((1,), (1,)), ((), ())), preferred_element_type=jnp.float32)

def block_slots(block_routes, expert_count, capacity):
    flat_routes = block_routes.reshape(-1).astype(jnp.int32)
    one_hot = (flat_routes[:, None] == jnp.arange(expert_count, dtype=jnp.int32)[None, :]).astype(jnp.int32)
    earlier = jnp.cumsum(one_hot, axis=0) - one_hot
    slot_index = lax.optimization_barrier(jnp.sum(earlier * one_hot, axis=1)).astype(jnp.int32)
    target = (flat_routes * capacity + slot_index).astype(jnp.int32)
    pair_count = flat_routes.shape[0]
    table = jnp.full((expert_count * capacity,), pair_count, jnp.int32).at[target].set(jnp.arange(pair_count, dtype=jnp.int32))
    return (target, table)

def gather_pairs(table, block_stream, block_upstream, block_weights, topk):
    token_of = table // topk
    zero_row = jnp.zeros((1, block_stream.shape[1]), jnp.bfloat16)
    stream_pad = jnp.concatenate([block_stream, zero_row], axis=0)
    upstream_pad = jnp.concatenate([block_upstream, zero_row], axis=0)
    weight_pad = jnp.concatenate([block_weights.reshape(-1), jnp.zeros((1,), jnp.float32)])
    send_rows = stream_pad[token_of]
    send_cot = (weight_pad[table][:, None] * upstream_pad[token_of].astype(jnp.float32)).astype(jnp.bfloat16)
    return (send_rows, send_cot)

def expert_backward(expert_rows, expert_cot, gate_weight, up_weight, down_weight):
    gate_pre = jnp.dot(expert_rows, gate_weight, preferred_element_type=jnp.float32)
    up_pre = jnp.dot(expert_rows, up_weight, preferred_element_type=jnp.float32)
    capped = jnp.minimum(gate_pre, clamp_limit)
    clipped = jnp.clip(up_pre, -clamp_limit, clamp_limit)
    gate_sigmoid = jax.nn.sigmoid(glu_alpha * capped)
    act = (capped * gate_sigmoid * (clipped + 1.0)).astype(jnp.bfloat16)
    grad_down = contract_rows(act, expert_cot)
    grad_act = times_transposed(expert_cot, down_weight)
    slope = gate_sigmoid + glu_alpha * capped * gate_sigmoid * (1.0 - gate_sigmoid)
    grad_gate_pre = jnp.where(gate_pre < clamp_limit, grad_act * (clipped + 1.0) * slope, 0.0).astype(jnp.bfloat16)
    grad_up_pre = jnp.where(jnp.abs(up_pre) < clamp_limit, grad_act * capped * gate_sigmoid, 0.0).astype(jnp.bfloat16)
    grad_gate = contract_rows(expert_rows, grad_gate_pre)
    grad_up = contract_rows(expert_rows, grad_up_pre)
    return (grad_gate, grad_up, grad_down, grad_gate_pre, grad_up_pre)

def one_expert(operands):
    expert_rows, expert_cot, gate_weight, up_weight, down_weight = operands
    grad_gate, grad_up, grad_down, grad_gate_pre, grad_up_pre = expert_backward(expert_rows, expert_cot, gate_weight, up_weight, down_weight)
    group_width = FF // N_TP
    gate_groups = grad_gate_pre.astype(jnp.float32).reshape(-1, N_TP, group_width)
    up_groups = grad_up_pre.astype(jnp.float32).reshape(-1, N_TP, group_width)
    gate_split = gate_weight.astype(jnp.float32).reshape(D, N_TP, group_width)
    up_split = up_weight.astype(jnp.float32).reshape(D, N_TP, group_width)
    partial_rows = jnp.einsum('rgf,dgf->grd', gate_groups, gate_split) + jnp.einsum('rgf,dgf->grd', up_groups, up_split)
    rounded = lax.optimization_barrier(partial_rows.astype(jnp.bfloat16))
    row_grad = lax.optimization_barrier(jnp.sum(rounded.astype(jnp.float32), axis=0)).astype(jnp.bfloat16)
    return (grad_gate, grad_up, grad_down, row_grad)

def take_rows(source_rows, target_rows):
    return source_rows[target_rows]

def reference(upstream, stream, routes, route_weights, glu_value, glu_gate, conv_taps, conv_saved, out_proj, expert_gate, expert_up, expert_down):
    block_routes = routes.reshape(N_SP, TOK_DEV, TOPK)
    targets, tables = jax.vmap(partial(block_slots, expert_count=EXPERTS, capacity=CAP))(block_routes)
    send_rows, send_cot = jax.vmap(partial(gather_pairs, topk=TOPK))(tables, stream.reshape(N_SP, TOK_DEV, D), upstream.reshape(N_SP, TOK_DEV, D), route_weights.reshape(N_SP, TOK_DEV, TOPK))
    expert_rows = send_rows.reshape(N_SP, EXPERTS, CAP, D).transpose(1, 0, 2, 3).reshape(EXPERTS, N_SP * CAP, D)
    expert_cot = send_cot.reshape(N_SP, EXPERTS, CAP, D).transpose(1, 0, 2, 3).reshape(EXPERTS, N_SP * CAP, D)
    grad_expert_gate, grad_expert_up, grad_expert_down, row_grads = lax.map(one_expert, (expert_rows, expert_cot, expert_gate, expert_up, expert_down))
    returned = row_grads.reshape(EXPERTS, N_SP, CAP, D).transpose(1, 0, 2, 3).reshape(N_SP, EXPERTS * CAP, D)
    pair_grads = jax.vmap(take_rows)(returned, targets)
    routed_sum = lax.optimization_barrier(jnp.sum(pair_grads.astype(jnp.float32).reshape(TOKENS, TOPK, D), axis=1))
    grad_stream = (upstream.astype(jnp.float32) + routed_sum).astype(jnp.bfloat16)
    saved_conv = conv_saved.astype(jnp.float32)
    mean_c = lax.optimization_barrier(jnp.mean(saved_conv, axis=1, keepdims=True))
    var_c = lax.optimization_barrier(jnp.mean(saved_conv * saved_conv, axis=1, keepdims=True)) - mean_c * mean_c
    inv_std = lax.rsqrt(var_c + norm_eps)
    normed = (saved_conv - mean_c) * inv_std
    norm_sigmoid = jax.nn.sigmoid(normed)
    mixed = (normed * norm_sigmoid).astype(jnp.bfloat16)
    grad_mixed = jnp.dot(grad_stream, out_proj, preferred_element_type=jnp.float32)
    grad_normed = grad_mixed * norm_sigmoid * (1.0 + normed * (1.0 - norm_sigmoid))
    first_mean = lax.optimization_barrier(jnp.mean(grad_normed, axis=1, keepdims=True))
    second_mean = lax.optimization_barrier(jnp.mean(grad_normed * normed, axis=1, keepdims=True))
    grad_conv = inv_std * (grad_normed - first_mean - normed * second_mean)
    padded = jnp.concatenate([grad_conv, jnp.zeros((KW - 1, CW), jnp.float32)], axis=0)
    grad_glu = jnp.zeros((TOKENS, CW), jnp.float32)
    for offset in range(KW):
        grad_glu = grad_glu + conv_taps[offset][None, :] * padded[offset:offset + TOKENS]
    gate_sig = jax.nn.sigmoid(glu_gate.astype(jnp.float32))
    grad_value = (grad_glu * gate_sig).astype(jnp.bfloat16)
    grad_gate = (grad_glu * glu_value.astype(jnp.float32) * gate_sig * (1.0 - gate_sig)).astype(jnp.bfloat16)
    grad_out_proj = contract_rows(grad_stream, mixed)
    return (grad_stream, grad_value, grad_gate, grad_out_proj, grad_expert_gate, grad_expert_up, grad_expert_down)
```

```python
import jax
import jax.numpy as jnp
from jax import lax
from jax.sharding import PartitionSpec as P


clamp_limit = 7.0
glu_alpha = 1.702
norm_eps = 1e-05


def passed_along(shard, axis, by):
    size = lax.axis_size(axis)
    pairs = [(i, i + by) for i in range(size) if 0 <= i + by < size]
    return lax.ppermute(shard, axis, pairs)


def contract_rows(left, right):
    return lax.dot_general(
        left, right, (((0,), (0,)), ((), ())), preferred_element_type=jnp.float32
    )


def times_transposed(left, right):
    return lax.dot_general(
        left, right, (((1,), (1,)), ((), ())), preferred_element_type=jnp.float32
    )


def pair_rows(block_routes, expert_count, capacity):
    tok_count, topk = block_routes.shape
    experts = jnp.arange(expert_count, dtype=jnp.int32)[None, :]
    hots = [(block_routes[:, k : k + 1] == experts).astype(jnp.float32) for k in range(topk)]
    before = (
        jnp.arange(tok_count)[:, None] > jnp.arange(tok_count)[None, :]
    ).astype(jnp.bfloat16)
    earlier = jnp.dot(before, sum(hots).astype(jnp.bfloat16), preferred_element_type=jnp.float32)
    slots = [jnp.sum(earlier * hot, axis=1).astype(jnp.int32) for hot in hots]
    return [block_routes[:, k] * capacity + slots[k] for k in range(topk)]


def select_pairs(targets, block_weights, row_count):
    rows = jnp.arange(row_count, dtype=jnp.int32)[:, None]
    hits = [target[None, :] == rows for target in targets]
    picks = sum(hit.astype(jnp.float32) for hit in hits).astype(jnp.bfloat16)
    row_weights = jnp.sum(
        sum(jnp.where(hit, block_weights[:, k][None, :], 0.0) for k, hit in enumerate(hits)), axis=1
    )
    return picks, row_weights


def expert_backward(expert_rows, expert_cot, gate_weight, up_weight, down_weight):
    gate_pre = jnp.dot(expert_rows, gate_weight, preferred_element_type=jnp.float32)
    up_pre = jnp.dot(expert_rows, up_weight, preferred_element_type=jnp.float32)
    capped = jnp.minimum(gate_pre, clamp_limit)
    clipped = jnp.clip(up_pre, -clamp_limit, clamp_limit)
    gate_sigmoid = jax.nn.sigmoid(glu_alpha * capped)
    act = (capped * gate_sigmoid * (clipped + 1.0)).astype(jnp.bfloat16)
    grad_down = contract_rows(act, expert_cot)
    grad_act = times_transposed(expert_cot, down_weight)
    slope = gate_sigmoid + glu_alpha * capped * gate_sigmoid * (1.0 - gate_sigmoid)
    grad_gate_pre = jnp.where(
        gate_pre < clamp_limit, grad_act * (clipped + 1.0) * slope, 0.0
    ).astype(jnp.bfloat16)
    grad_up_pre = jnp.where(
        jnp.abs(up_pre) < clamp_limit, grad_act * capped * gate_sigmoid, 0.0
    ).astype(jnp.bfloat16)
    grad_gate = contract_rows(expert_rows, grad_gate_pre)
    grad_up = contract_rows(expert_rows, grad_up_pre)
    return (grad_gate, grad_up, grad_down, grad_gate_pre, grad_up_pre)


def on_device(
    upstream,
    stream,
    routes,
    route_weights,
    glu_value,
    glu_gate,
    conv_taps,
    conv_saved,
    out_proj,
    expert_gate,
    expert_up,
    expert_down,
):
    tok_count = upstream.shape[0]
    model_width = upstream.shape[1]
    expert_count = lax.axis_size("sp")
    capacity = 4 * tok_count // expert_count
    slice_width = model_width // lax.axis_size("tp")
    column_start = lax.axis_index("tp") * slice_width
    targets = pair_rows(routes, expert_count, capacity)
    picks, row_weights = select_pairs(targets, route_weights, expert_count * capacity)
    stream_part = lax.dynamic_slice_in_dim(stream, column_start, slice_width, 1)
    upstream_part = lax.dynamic_slice_in_dim(upstream, column_start, slice_width, 1)
    send_rows = jnp.dot(picks, stream_part, preferred_element_type=jnp.float32).astype(jnp.bfloat16)
    send_cot = (
        row_weights[:, None] * jnp.dot(picks, upstream_part, preferred_element_type=jnp.float32)
    ).astype(jnp.bfloat16)
    part_shape = (expert_count, capacity, slice_width)
    part_rows, part_cot = (
        lax.all_to_all(
            send_rows.reshape(part_shape), "sp", split_axis=0, concat_axis=0, tiled=True
        ),
        lax.all_to_all(send_cot.reshape(part_shape), "sp", split_axis=0, concat_axis=0, tiled=True),
    )
    got_rows, got_cot = (
        lax.all_gather(part_rows, "tp", axis=2, tiled=True),
        lax.all_gather(part_cot, "tp", axis=2, tiled=True),
    )
    expert_rows = got_rows.reshape(-1, model_width)
    expert_cot = got_cot.reshape(-1, model_width)
    gate_weight = expert_gate[0]
    up_weight = expert_up[0]
    down_weight = expert_down[0]
    grad_gate_w, grad_up_w, grad_down_w, grad_gate_pre, grad_up_pre = expert_backward(
        expert_rows, expert_cot, gate_weight, up_weight, down_weight
    )
    partial_rows = times_transposed(grad_gate_pre, gate_weight) + times_transposed(
        grad_up_pre, up_weight
    )
    summed_rows = lax.psum_scatter(
        partial_rows.astype(jnp.bfloat16), "tp", scatter_dimension=1, tiled=True
    )
    returned = lax.all_to_all(
        summed_rows.reshape(expert_count, capacity, slice_width),
        "sp",
        split_axis=0,
        concat_axis=0,
        tiled=True,
    )
    routed_sum = contract_rows(picks, returned.reshape(expert_count * capacity, slice_width))
    upstream_own = lax.dynamic_slice_in_dim(upstream, column_start, slice_width, 1)
    grad_stream = (upstream_own.astype(jnp.float32) + routed_sum).astype(jnp.bfloat16)
    full_grad = lax.all_gather(grad_stream, "tp", axis=1, tiled=True)
    conv_width = conv_saved.shape[1] * lax.axis_size("tp")
    saved_conv = conv_saved.astype(jnp.float32)
    total_sum, square_sum = lax.psum(
        (jnp.sum(saved_conv, axis=1), jnp.sum(saved_conv * saved_conv, axis=1)), "tp"
    )
    mean_c = (total_sum / conv_width)[:, None]
    var_c = (square_sum / conv_width)[:, None] - mean_c * mean_c
    inv_std = lax.rsqrt(var_c + norm_eps)
    normed = (saved_conv - mean_c) * inv_std
    norm_sigmoid = jax.nn.sigmoid(normed)
    mixed = (normed * norm_sigmoid).astype(jnp.bfloat16)
    grad_mixed = jnp.dot(full_grad, out_proj, preferred_element_type=jnp.float32)
    grad_normed = grad_mixed * norm_sigmoid * (1.0 + normed * (1.0 - norm_sigmoid))
    first_sum, second_sum = lax.psum(
        (jnp.sum(grad_normed, axis=1), jnp.sum(grad_normed * normed, axis=1)), "tp"
    )
    grad_conv = inv_std * (
        grad_normed - (first_sum / conv_width)[:, None] - normed * (second_sum / conv_width)[:, None]
    )
    kernel_width = conv_taps.shape[0]
    rim_rows = passed_along(grad_conv[: kernel_width - 1], "sp", -1)
    padded = jnp.concatenate([grad_conv, rim_rows], axis=0)
    grad_glu = jnp.zeros_like(grad_conv)
    for offset in range(kernel_width):
        grad_glu = grad_glu + conv_taps[offset][None, :] * padded[offset : offset + tok_count]
    gate_sig = jax.nn.sigmoid(glu_gate.astype(jnp.float32))
    grad_value = (grad_glu * gate_sig).astype(jnp.bfloat16)
    grad_gate = (grad_glu * glu_value.astype(jnp.float32) * gate_sig * (1.0 - gate_sig)).astype(
        jnp.bfloat16
    )
    proj_parts = contract_rows(full_grad, mixed).astype(jnp.bfloat16)
    proj_parts = lax.all_to_all(
        proj_parts.reshape(expert_count, -1, mixed.shape[1]),
        "sp",
        split_axis=0,
        concat_axis=0,
        tiled=True,
    )
    grad_out_proj = jnp.sum(proj_parts.astype(jnp.float32), axis=0)
    return (
        grad_stream,
        grad_value,
        grad_gate,
        grad_out_proj,
        grad_gate_w[None],
        grad_up_w[None],
        grad_down_w[None],
    )


def solution(mesh):
    in_specs = (
        P("sp", None),
        P("sp", None),
        P("sp", None),
        P("sp", None),
        P("sp", "tp"),
        P("sp", "tp"),
        P(None, "tp"),
        P("sp", "tp"),
        P(None, "tp"),
        P("sp", None, "tp"),
        P("sp", None, "tp"),
        P("sp", "tp", None),
    )
    out_specs = (
        P("sp", "tp"),
        P("sp", "tp"),
        P("sp", "tp"),
        P("sp", "tp"),
        P("sp", None, "tp"),
        P("sp", None, "tp"),
        P("sp", "tp", None),
    )
    return jax.shard_map(
        on_device, mesh=mesh, in_specs=in_specs, out_specs=out_specs, check_vma=False
    )
```

```python
import functools

import jax
import jax.numpy as jnp
from jax import lax
from jax.experimental import pallas as pl
from jax.experimental.pallas import tpu as pltpu
from jax.sharding import PartitionSpec as P


clamp_limit = 7.0
glu_alpha = 1.702
norm_eps = 1e-05


def passed_along(shard, axis, by):
    size = lax.axis_size(axis)
    pairs = [(i, i + by) for i in range(size) if 0 <= i + by < size]
    return lax.ppermute(shard, axis, pairs)


def contract_rows(left, right):
    return lax.dot_general(
        left, right, (((0,), (0,)), ((), ())), preferred_element_type=jnp.float32
    )


def times_transposed(left, right):
    return lax.dot_general(
        left, right, (((1,), (1,)), ((), ())), preferred_element_type=jnp.float32
    )


def pair_rows(block_routes, expert_count, capacity):
    tok_count, topk = block_routes.shape
    experts = jnp.arange(expert_count, dtype=jnp.int32)[None, :]
    hots = [(block_routes[:, k : k + 1] == experts).astype(jnp.float32) for k in range(topk)]
    before = (
        jnp.arange(tok_count)[:, None] > jnp.arange(tok_count)[None, :]
    ).astype(jnp.bfloat16)
    earlier = jnp.dot(before, sum(hots).astype(jnp.bfloat16), preferred_element_type=jnp.float32)
    slots = [jnp.sum(earlier * hot, axis=1).astype(jnp.int32) for hot in hots]
    return [block_routes[:, k] * capacity + slots[k] for k in range(topk)]


def select_pairs(targets, block_weights, row_count):
    rows = jnp.arange(row_count, dtype=jnp.int32)[:, None]
    hits = [target[None, :] == rows for target in targets]
    picks = sum(hit.astype(jnp.float32) for hit in hits).astype(jnp.bfloat16)
    row_weights = jnp.sum(
        sum(jnp.where(hit, block_weights[:, k][None, :], 0.0) for k, hit in enumerate(hits)), axis=1
    )
    return picks, row_weights


def greet(sp_count, tp_count):
    me, lane = lax.axis_index("sp"), lax.axis_index("tp")
    barrier = pltpu.get_barrier_semaphore()
    for step in range(1, sp_count):
        pl.semaphore_signal(
            barrier,
            inc=1,
            device_id={"sp": lax.rem(me + step, sp_count)},
            device_id_type=pl.DeviceIdType.MESH,
        )
    for step in range(1, tp_count):
        pl.semaphore_signal(
            barrier,
            inc=1,
            device_id={"tp": lax.rem(lane + step, tp_count)},
            device_id_type=pl.DeviceIdType.MESH,
        )
    pl.semaphore_wait(barrier, sp_count + tp_count - 2)


def remote(src, dst, send_sem, recv_sem, **target):
    return pltpu.make_async_remote_copy(
        src_ref=src,
        dst_ref=dst,
        send_sem=send_sem,
        recv_sem=recv_sem,
        device_id=target,
        device_id_type=pl.DeviceIdType.MESH,
    )


def dispatch_kernel(
    sp_count,
    tp_count,
    rows_ref,
    cot_ref,
    got_rows,
    got_cot,
    far_send,
    far_recv,
    side_send,
    side_recv,
    pair_send,
    pair_recv,
    own_sem,
):
    me, lane = lax.axis_index("sp"), lax.axis_index("tp")
    width = rows_ref.shape[2]
    chips = tp_count // 2
    partner = lane + 1 - 2 * lax.rem(lane, 2)
    sources, results = (rows_ref, cot_ref), (got_rows, got_cot)

    def place(which, block, column):
        return results[which].at[block, :, pl.ds(pl.multiple_of(column * width, width), width)]

    greet(sp_count, tp_count)

    def far(which, step):
        to = lax.rem(me + step, sp_count)
        return remote(
            sources[which].at[to],
            place(which, me, lane),
            far_send.at[which, step],
            far_recv.at[which, step],
            sp=to,
        )

    def beside(which, step, hop):
        block = lax.rem(me + sp_count - step, sp_count)
        source = sources[which].at[me] if step == 0 else place(which, block, lane)
        return remote(
            source,
            place(which, block, lane),
            side_send.at[which, step, hop],
            side_recv.at[which, step, hop],
            tp=lax.rem(lane + 2 * hop, tp_count),
        )

    def paired(which, step, hop):
        block = lax.rem(me + sp_count - step, sp_count)
        column = lax.rem(lane + tp_count - 2 * hop, tp_count)
        source = (
            sources[which].at[me] if step == 0 and hop == 0 else place(which, block, column)
        )
        return remote(
            source,
            place(which, block, column),
            pair_send.at[which, step, hop],
            pair_recv.at[which, step, hop],
            tp=partner,
        )

    started = []

    def begin(copy):
        copy.start()
        started.append(copy)

    order = [(which, step) for which in range(2) for step in range(1, sp_count)]
    own = [
        pltpu.make_async_copy(sources[which].at[me], place(which, me, lane), own_sem.at[which])
        for which in range(2)
    ]
    for which in range(2):
        own[which].start()
        for step in range(1, sp_count):
            begin(far(which, step))
    arrivals = []
    for which in range(2):
        arrivals += [(which, step) for step in range(sp_count)]
    lag = 2
    for at in range(len(arrivals) + lag):
        if at < len(arrivals):
            which, step = arrivals[at]
            if step:
                far(which, step).wait_recv()
            for hop in range(1, chips):
                begin(beside(which, step, hop))
            begin(paired(which, step, 0))
        if at >= lag:
            which, step = arrivals[at - lag]
            for hop in range(1, chips):
                beside(which, step, hop).wait_recv()
                begin(paired(which, step, hop))
    for which, step in arrivals:
        for hop in range(chips):
            paired(which, step, hop).wait_recv()
    for copy in started:
        copy.wait_send()
    for copy in own:
        copy.wait()


def dispatch(send_rows, send_cot, sp_count, tp_count):
    blocks, capacity, width = send_rows.shape
    full = jax.ShapeDtypeStruct((blocks, capacity, width * tp_count), send_rows.dtype)
    dma = pltpu.SemaphoreType.DMA
    chips = tp_count // 2
    return pl.pallas_call(
        functools.partial(dispatch_kernel, sp_count, tp_count),
        out_shape=(full, full),
        in_specs=[pl.BlockSpec(memory_space=pltpu.VMEM)] * 2,
        out_specs=[pl.BlockSpec(memory_space=pl.ANY)] * 2,
        scratch_shapes=[dma((2, sp_count))] * 2
        + [dma((2, sp_count, chips))] * 4
        + [dma((2,))],
        compiler_params=pltpu.CompilerParams(collective_id=0, has_side_effects=True),
        name="dispatch",
    )(send_rows, send_cot)


def return_kernel(
    sp_count,
    tp_count,
    partial_ref,
    out_ref,
    pair_in,
    side_out,
    side_in,
    total,
    pair_send,
    pair_recv,
    side_send,
    side_recv,
    far_send,
    far_recv,
):
    me, lane = lax.axis_index("sp"), lax.axis_index("tp")
    width = out_ref.shape[2]
    chips = tp_count // 2
    core = lax.rem(lane, 2)
    partner = lane + 1 - 2 * core

    greet(sp_count, tp_count)
    started = []

    def begin(copy):
        copy.start()
        started.append(copy)

    def columns(column):
        return pl.ds(pl.multiple_of(column * width, width), width)

    def swapped(step, hop):
        block = lax.rem(me + step, sp_count)
        chip_lane = lax.rem(lane + 2 * hop, tp_count)
        other = chip_lane + 1 - 2 * core
        return remote(
            partial_ref.at[block, :, columns(other)],
            pair_in.at[step, hop],
            pair_send.at[step, hop],
            pair_recv.at[step, hop],
            tp=partner,
        )

    def beside(step, hop):
        return remote(
            side_out.at[step, hop - 1],
            side_in.at[step, hop - 1],
            side_send.at[step, hop - 1],
            side_recv.at[step, hop - 1],
            tp=lax.rem(lane + 2 * hop, tp_count),
        )

    def far(step):
        return remote(
            total.at[step],
            out_ref.at[me],
            far_send.at[step],
            far_recv.at[step],
            sp=lax.rem(me + step, sp_count),
        )

    order = list(range(1, sp_count)) + [0]
    for step in order:
        for hop in list(range(1, chips)) + [0]:
            begin(swapped(step, hop))

    def pair_sum(step, hop):
        block = lax.rem(me + step, sp_count)
        column = lax.rem(lane + 2 * hop, tp_count)
        return partial_ref[block, :, columns(column)].astype(jnp.float32) + pair_in[
            step, hop
        ].astype(jnp.float32)

    lag = 2
    for at in range(sp_count + lag):
        if at < sp_count:
            step = order[at]
            for hop in range(1, chips):
                swapped(step, hop).wait_recv()
                side_out[step, hop - 1] = pair_sum(step, hop).astype(jnp.bfloat16)
                begin(beside(step, hop))
        if at >= lag:
            step = order[at - lag]
            swapped(step, 0).wait_recv()
            value = pair_sum(step, 0)
            for hop in range(1, chips):
                beside(step, hop).wait_recv()
                value += side_in[step, hop - 1].astype(jnp.float32)
            if step:
                total[step] = value.astype(jnp.bfloat16)
                begin(far(step))
            else:
                out_ref[me] = value.astype(jnp.bfloat16)
    for step in range(1, sp_count):
        far(step).wait_recv()
    for copy in started:
        copy.wait_send()


def send_back(partial_rows, sp_count, tp_count):
    blocks, capacity, model_width = partial_rows.shape
    width = model_width // tp_count
    chips = tp_count // 2
    dma, vmem = pltpu.SemaphoreType.DMA, pltpu.VMEM
    return pl.pallas_call(
        functools.partial(return_kernel, sp_count, tp_count),
        out_shape=jax.ShapeDtypeStruct((blocks, capacity, width), jnp.bfloat16),
        in_specs=[pl.BlockSpec(memory_space=vmem)],
        out_specs=pl.BlockSpec(memory_space=vmem),
        scratch_shapes=[
            vmem((sp_count, chips, capacity, width), jnp.bfloat16),
            vmem((sp_count, chips - 1, capacity, width), jnp.bfloat16),
            vmem((sp_count, chips - 1, capacity, width), jnp.bfloat16),
            vmem((sp_count, capacity, width), jnp.bfloat16),
            dma((sp_count, chips)),
            dma((sp_count, chips)),
            dma((sp_count, chips - 1)),
            dma((sp_count, chips - 1)),
            dma((sp_count,)),
            dma((sp_count,)),
        ],
        compiler_params=pltpu.CompilerParams(collective_id=1, has_side_effects=True),
        name="send_back",
    )(partial_rows)


def expert_backward(expert_rows, expert_cot, gate_weight, up_weight, down_weight):
    gate_pre = jnp.dot(expert_rows, gate_weight, preferred_element_type=jnp.float32)
    up_pre = jnp.dot(expert_rows, up_weight, preferred_element_type=jnp.float32)
    capped = jnp.minimum(gate_pre, clamp_limit)
    clipped = jnp.clip(up_pre, -clamp_limit, clamp_limit)
    gate_sigmoid = jax.nn.sigmoid(glu_alpha * capped)
    act = (capped * gate_sigmoid * (clipped + 1.0)).astype(jnp.bfloat16)
    grad_down = contract_rows(act, expert_cot)
    grad_act = times_transposed(expert_cot, down_weight)
    slope = gate_sigmoid + glu_alpha * capped * gate_sigmoid * (1.0 - gate_sigmoid)
    grad_gate_pre = jnp.where(
        gate_pre < clamp_limit, grad_act * (clipped + 1.0) * slope, 0.0
    ).astype(jnp.bfloat16)
    grad_up_pre = jnp.where(
        jnp.abs(up_pre) < clamp_limit, grad_act * capped * gate_sigmoid, 0.0
    ).astype(jnp.bfloat16)
    grad_gate = contract_rows(expert_rows, grad_gate_pre)
    grad_up = contract_rows(expert_rows, grad_up_pre)
    return (grad_gate, grad_up, grad_down, grad_gate_pre, grad_up_pre)


def on_device(
    upstream,
    stream,
    routes,
    route_weights,
    glu_value,
    glu_gate,
    conv_taps,
    conv_saved,
    out_proj,
    expert_gate,
    expert_up,
    expert_down,
):
    tok_count = upstream.shape[0]
    model_width = upstream.shape[1]
    expert_count = lax.axis_size("sp")
    capacity = 4 * tok_count // expert_count
    slice_width = model_width // lax.axis_size("tp")
    column_start = lax.axis_index("tp") * slice_width
    targets = pair_rows(routes, expert_count, capacity)
    picks, row_weights = select_pairs(targets, route_weights, expert_count * capacity)
    stream_part = lax.dynamic_slice_in_dim(stream, column_start, slice_width, 1)
    upstream_part = lax.dynamic_slice_in_dim(upstream, column_start, slice_width, 1)
    send_rows = jnp.dot(picks, stream_part, preferred_element_type=jnp.float32).astype(jnp.bfloat16)
    send_cot = (
        row_weights[:, None] * jnp.dot(picks, upstream_part, preferred_element_type=jnp.float32)
    ).astype(jnp.bfloat16)
    part_shape = (expert_count, capacity, slice_width)
    got_rows, got_cot = dispatch(
        send_rows.reshape(part_shape),
        send_cot.reshape(part_shape),
        expert_count,
        lax.axis_size("tp"),
    )
    expert_rows = got_rows.reshape(-1, model_width)
    expert_cot = got_cot.reshape(-1, model_width)
    gate_weight = expert_gate[0]
    up_weight = expert_up[0]
    down_weight = expert_down[0]
    grad_gate_w, grad_up_w, grad_down_w, grad_gate_pre, grad_up_pre = expert_backward(
        expert_rows, expert_cot, gate_weight, up_weight, down_weight
    )
    partial_rows = times_transposed(grad_gate_pre, gate_weight) + times_transposed(
        grad_up_pre, up_weight
    )
    returned = send_back(
        partial_rows.astype(jnp.bfloat16).reshape(expert_count, capacity, model_width),
        expert_count,
        lax.axis_size("tp"),
    )
    routed_sum = contract_rows(picks, returned.reshape(expert_count * capacity, slice_width))
    upstream_own = lax.dynamic_slice_in_dim(upstream, column_start, slice_width, 1)
    grad_stream = (upstream_own.astype(jnp.float32) + routed_sum).astype(jnp.bfloat16)
    full_grad = lax.all_gather(grad_stream, "tp", axis=1, tiled=True)
    conv_width = conv_saved.shape[1] * lax.axis_size("tp")
    saved_conv = conv_saved.astype(jnp.float32)
    total_sum, square_sum = lax.psum(
        (jnp.sum(saved_conv, axis=1), jnp.sum(saved_conv * saved_conv, axis=1)), "tp"
    )
    mean_c = (total_sum / conv_width)[:, None]
    var_c = (square_sum / conv_width)[:, None] - mean_c * mean_c
    inv_std = lax.rsqrt(var_c + norm_eps)
    normed = (saved_conv - mean_c) * inv_std
    norm_sigmoid = jax.nn.sigmoid(normed)
    mixed = (normed * norm_sigmoid).astype(jnp.bfloat16)
    grad_mixed = jnp.dot(full_grad, out_proj, preferred_element_type=jnp.float32)
    grad_normed = grad_mixed * norm_sigmoid * (1.0 + normed * (1.0 - norm_sigmoid))
    first_sum, second_sum = lax.psum(
        (jnp.sum(grad_normed, axis=1), jnp.sum(grad_normed * normed, axis=1)), "tp"
    )
    grad_conv = inv_std * (
        grad_normed - (first_sum / conv_width)[:, None] - normed * (second_sum / conv_width)[:, None]
    )
    kernel_width = conv_taps.shape[0]
    rim_rows = passed_along(grad_conv[: kernel_width - 1], "sp", -1)
    padded = jnp.concatenate([grad_conv, rim_rows], axis=0)
    grad_glu = jnp.zeros_like(grad_conv)
    for offset in range(kernel_width):
        grad_glu = grad_glu + conv_taps[offset][None, :] * padded[offset : offset + tok_count]
    gate_sig = jax.nn.sigmoid(glu_gate.astype(jnp.float32))
    grad_value = (grad_glu * gate_sig).astype(jnp.bfloat16)
    grad_gate = (grad_glu * glu_value.astype(jnp.float32) * gate_sig * (1.0 - gate_sig)).astype(
        jnp.bfloat16
    )
    proj_parts = contract_rows(full_grad, mixed).astype(jnp.bfloat16)
    proj_parts = lax.all_to_all(
        proj_parts.reshape(expert_count, -1, mixed.shape[1]),
        "sp",
        split_axis=0,
        concat_axis=0,
        tiled=True,
    )
    grad_out_proj = jnp.sum(proj_parts.astype(jnp.float32), axis=0)
    return (
        grad_stream,
        grad_value,
        grad_gate,
        grad_out_proj,
        grad_gate_w[None],
        grad_up_w[None],
        grad_down_w[None],
    )


def solution(mesh):
    in_specs = (
        P("sp", None),
        P("sp", None),
        P("sp", None),
        P("sp", None),
        P("sp", "tp"),
        P("sp", "tp"),
        P(None, "tp"),
        P("sp", "tp"),
        P(None, "tp"),
        P("sp", None, "tp"),
        P("sp", None, "tp"),
        P("sp", "tp", None),
    )
    out_specs = (
        P("sp", "tp"),
        P("sp", "tp"),
        P("sp", "tp"),
        P("sp", "tp"),
        P("sp", None, "tp"),
        P("sp", None, "tp"),
        P("sp", "tp", None),
    )
    return jax.shard_map(
        on_device, mesh=mesh, in_specs=in_specs, out_specs=out_specs, check_vma=False
    )
```

```python
import functools

import jax
import jax.numpy as jnp
from jax import lax
from jax.experimental import pallas as pl
from jax.experimental.pallas import tpu as pltpu
from jax.sharding import PartitionSpec as P


clamp_limit = 7.0
glu_alpha = 1.702
norm_eps = 1e-05


def contract_rows(left, right):
    return lax.dot_general(
        left, right, (((0,), (0,)), ((), ())), preferred_element_type=jnp.float32
    )


def times_transposed(left, right):
    return lax.dot_general(
        left, right, (((1,), (1,)), ((), ())), preferred_element_type=jnp.float32
    )


def pair_rows(block_routes, expert_count, capacity):
    tok_count, topk = block_routes.shape
    experts = jnp.arange(expert_count, dtype=jnp.int32)[None, :]
    hots = [(block_routes[:, k : k + 1] == experts).astype(jnp.float32) for k in range(topk)]
    before = (
        jnp.arange(tok_count)[:, None] > jnp.arange(tok_count)[None, :]
    ).astype(jnp.bfloat16)
    earlier = jnp.dot(before, sum(hots).astype(jnp.bfloat16), preferred_element_type=jnp.float32)
    slots = [jnp.sum(earlier * hot, axis=1).astype(jnp.int32) for hot in hots]
    return [block_routes[:, k] * capacity + slots[k] for k in range(topk)]


def select_pairs(targets, block_weights, row_count):
    rows = jnp.arange(row_count, dtype=jnp.int32)[:, None]
    hits = [target[None, :] == rows for target in targets]
    picks = sum(hit.astype(jnp.float32) for hit in hits).astype(jnp.bfloat16)
    row_weights = jnp.sum(
        sum(jnp.where(hit, block_weights[:, k][None, :], 0.0) for k, hit in enumerate(hits)), axis=1
    )
    return picks, row_weights


def greet(sp_count, tp_count):
    me, lane = lax.axis_index("sp"), lax.axis_index("tp")
    barrier = pltpu.get_barrier_semaphore()
    for step in range(1, sp_count):
        pl.semaphore_signal(
            barrier,
            inc=1,
            device_id={"sp": lax.rem(me + step, sp_count)},
            device_id_type=pl.DeviceIdType.MESH,
        )
    for step in range(1, tp_count):
        pl.semaphore_signal(
            barrier,
            inc=1,
            device_id={"tp": lax.rem(lane + step, tp_count)},
            device_id_type=pl.DeviceIdType.MESH,
        )
    pl.semaphore_wait(barrier, sp_count + tp_count - 2)


def remote(src, dst, send_sem, recv_sem, **target):
    return pltpu.make_async_remote_copy(
        src_ref=src,
        dst_ref=dst,
        send_sem=send_sem,
        recv_sem=recv_sem,
        device_id=target,
        device_id_type=pl.DeviceIdType.MESH,
    )


def dispatch_kernel(
    sp_count,
    tp_count,
    rows_ref,
    cot_ref,
    got_rows,
    got_cot,
    far_send,
    far_recv,
    side_send,
    side_recv,
    pair_send,
    pair_recv,
    own_sem,
):
    me, lane = lax.axis_index("sp"), lax.axis_index("tp")
    width = rows_ref.shape[2]
    chips = tp_count // 2
    partner = lane + 1 - 2 * lax.rem(lane, 2)
    sources, results = (rows_ref, cot_ref), (got_rows, got_cot)

    def place(which, block, column):
        return results[which].at[block, :, pl.ds(pl.multiple_of(column * width, width), width)]

    greet(sp_count, tp_count)

    def far(which, step):
        to = lax.rem(me + step, sp_count)
        return remote(
            sources[which].at[to],
            place(which, me, lane),
            far_send.at[which, step],
            far_recv.at[which, step],
            sp=to,
        )

    def beside(which, step, hop):
        block = lax.rem(me + sp_count - step, sp_count)
        source = sources[which].at[me] if step == 0 else place(which, block, lane)
        return remote(
            source,
            place(which, block, lane),
            side_send.at[which, step, hop],
            side_recv.at[which, step, hop],
            tp=lax.rem(lane + 2 * hop, tp_count),
        )

    def paired(which, step, hop):
        block = lax.rem(me + sp_count - step, sp_count)
        column = lax.rem(lane + tp_count - 2 * hop, tp_count)
        source = (
            sources[which].at[me] if step == 0 and hop == 0 else place(which, block, column)
        )
        return remote(
            source,
            place(which, block, column),
            pair_send.at[which, step, hop],
            pair_recv.at[which, step, hop],
            tp=partner,
        )

    started = []

    def begin(copy):
        copy.start()
        started.append(copy)

    order = [(which, step) for which in range(2) for step in range(1, sp_count)]
    own = [
        pltpu.make_async_copy(sources[which].at[me], place(which, me, lane), own_sem.at[which])
        for which in range(2)
    ]
    for which in range(2):
        own[which].start()
        for step in range(1, sp_count):
            begin(far(which, step))
    arrivals = []
    for which in range(2):
        arrivals += [(which, step) for step in range(sp_count)]
    lag = 2
    for at in range(len(arrivals) + lag):
        if at < len(arrivals):
            which, step = arrivals[at]
            if step:
                far(which, step).wait_recv()
            for hop in range(1, chips):
                begin(beside(which, step, hop))
            begin(paired(which, step, 0))
        if at >= lag:
            which, step = arrivals[at - lag]
            for hop in range(1, chips):
                beside(which, step, hop).wait_recv()
                begin(paired(which, step, hop))
    for which, step in arrivals:
        for hop in range(chips):
            paired(which, step, hop).wait_recv()
    for copy in started:
        copy.wait_send()
    for copy in own:
        copy.wait()


def dispatch(send_rows, send_cot, sp_count, tp_count):
    blocks, capacity, width = send_rows.shape
    full = jax.ShapeDtypeStruct((blocks, capacity, width * tp_count), send_rows.dtype)
    dma = pltpu.SemaphoreType.DMA
    chips = tp_count // 2
    return pl.pallas_call(
        functools.partial(dispatch_kernel, sp_count, tp_count),
        out_shape=(full, full),
        in_specs=[pl.BlockSpec(memory_space=pltpu.VMEM)] * 2,
        out_specs=[pl.BlockSpec(memory_space=pl.ANY)] * 2,
        scratch_shapes=[dma((2, sp_count))] * 2
        + [dma((2, sp_count, chips))] * 4
        + [dma((2,))],
        compiler_params=pltpu.CompilerParams(collective_id=0, has_side_effects=True),
        name="dispatch",
    )(send_rows, send_cot)


def tail_kernel(
    sp_count,
    tp_count,
    partial_ref,
    picks_ref,
    upstream_ref,
    saved_ref,
    proj_ref,
    taps_ref,
    value_ref,
    gate_ref,
    grad_stream_ref,
    grad_value_ref,
    grad_gate_ref,
    grad_proj_ref,
    pair_in,
    side_out,
    side_in,
    total,
    returned,
    full,
    stat_out,
    stat_in,
    parts_out,
    parts_in,
    rim_in,
    padded,
    pair_send,
    pair_recv,
    side_send,
    side_recv,
    far_send,
    far_recv,
    full_send,
    full_recv,
    stat_send,
    stat_recv,
    parts_send,
    parts_recv,
    rim_send,
    rim_recv,
):
    me, lane = lax.axis_index("sp"), lax.axis_index("tp")
    width = returned.shape[2]
    chips = tp_count // 2
    core = lax.rem(lane, 2)
    partner = lane + 1 - 2 * core
    tok_count, channels = saved_ref.shape
    conv_width = channels * tp_count
    groups = tok_count // 128
    f32, bf16 = jnp.float32, jnp.bfloat16

    greet(sp_count, tp_count)
    started = []

    def begin(copy):
        copy.start()
        started.append(copy)

    def columns(column):
        return pl.ds(pl.multiple_of(column * width, width), width)

    def swapped(step, hop):
        block = lax.rem(me + step, sp_count)
        other = lax.rem(lane + 2 * hop, tp_count) + 1 - 2 * core
        return remote(
            partial_ref.at[block, :, columns(other)],
            pair_in.at[step, hop],
            pair_send.at[step, hop],
            pair_recv.at[step, hop],
            tp=partner,
        )

    def beside(step, hop):
        return remote(
            side_out.at[step, hop - 1],
            side_in.at[step, hop - 1],
            side_send.at[step, hop - 1],
            side_recv.at[step, hop - 1],
            tp=lax.rem(lane + 2 * hop, tp_count),
        )

    def far(step):
        return remote(
            total.at[step],
            returned.at[me],
            far_send.at[step],
            far_recv.at[step],
            sp=lax.rem(me + step, sp_count),
        )

    order = list(range(1, sp_count)) + [0]
    for step in order:
        for hop in list(range(1, chips)) + [0]:
            begin(swapped(step, hop))

    eye = (
        lax.broadcasted_iota(jnp.int32, (128, 128), 0)
        == lax.broadcasted_iota(jnp.int32, (128, 128), 1)
    )

    def stat(phase, hop):
        return remote(
            stat_out.at[phase],
            stat_in.at[phase, hop],
            stat_send.at[phase, hop],
            stat_recv.at[phase, hop],
            tp=lax.rem(lane + hop, tp_count),
        )

    def share(phase, sums):
        stat_out[phase] = jnp.zeros(stat_out.shape[1:], f32)
        row = 0
        for item in sums:
            for group in range(groups):
                part = item[group * 128 : (group + 1) * 128]
                spread = jnp.where(eye, jnp.broadcast_to(part, (128, 128)), 0.0)
                stat_out[phase, row : row + 1] = jnp.sum(spread, axis=0, keepdims=True)
                row += 1
        for hop in range(1, tp_count):
            begin(stat(phase, hop))

    def shared(phase):
        value = stat_out[phase]
        for hop in range(1, tp_count):
            stat(phase, hop).wait_recv()
            value += stat_in[phase, hop]
        columns_of = []
        for item in range(2):
            parts = []
            for group in range(groups):
                row = item * groups + group
                spread = jnp.broadcast_to(value[row : row + 1], (128, 128))
                parts.append(jnp.sum(jnp.where(eye, spread, 0.0), axis=1, keepdims=True))
            columns_of.append(jnp.concatenate(parts, axis=0))
        return columns_of

    saved_conv = saved_ref[...].astype(f32)
    share(
        0,
        (
            jnp.sum(saved_conv, axis=1, keepdims=True),
            jnp.sum(saved_conv * saved_conv, axis=1, keepdims=True),
        ),
    )

    def pair_sum(step, hop):
        block = lax.rem(me + step, sp_count)
        column = lax.rem(lane + 2 * hop, tp_count)
        return partial_ref[block, :, columns(column)].astype(f32) + pair_in[step, hop].astype(f32)

    lag = 2
    for at in range(sp_count + lag):
        if at < sp_count:
            step = order[at]
            for hop in range(1, chips):
                swapped(step, hop).wait_recv()
                side_out[step, hop - 1] = pair_sum(step, hop).astype(bf16)
                begin(beside(step, hop))
        if at >= lag:
            step = order[at - lag]
            swapped(step, 0).wait_recv()
            value = pair_sum(step, 0)
            for hop in range(1, chips):
                beside(step, hop).wait_recv()
                value += side_in[step, hop - 1].astype(f32)
            if step:
                total[step] = value.astype(bf16)
                begin(far(step))
            else:
                returned[me] = value.astype(bf16)

    total_sum, square_sum = shared(0)
    mean_c = total_sum / conv_width
    var_c = square_sum / conv_width - mean_c * mean_c
    inv_std = lax.rsqrt(var_c + norm_eps)
    normed = (saved_conv - mean_c) * inv_std
    norm_sigmoid = jax.nn.sigmoid(normed)
    mixed = (normed * norm_sigmoid).astype(bf16)

    for step in range(1, sp_count):
        far(step).wait_recv()
    routed_sum = jnp.dot(
        picks_ref[...],
        returned[...].reshape(-1, width),
        preferred_element_type=f32,
    )
    own_grad = (upstream_ref[...].astype(f32) + routed_sum).astype(bf16)
    grad_stream_ref[...] = own_grad
    full[:, columns(lane)] = own_grad

    def spread_full(hop):
        return remote(
            full.at[:, columns(lane)],
            full.at[:, columns(lane)],
            full_send.at[0, hop],
            full_recv.at[0, hop],
            tp=lax.rem(lane + 2 * hop, tp_count),
        )

    def hand_over(hop):
        column = lax.rem(lane + tp_count - 2 * hop, tp_count)
        return remote(
            full.at[:, columns(column)],
            full.at[:, columns(column)],
            full_send.at[1, hop],
            full_recv.at[1, hop],
            tp=partner,
        )

    for hop in range(1, chips):
        begin(spread_full(hop))
    begin(hand_over(0))
    for hop in range(1, chips):
        spread_full(hop).wait_recv()
        begin(hand_over(hop))
    for hop in range(chips):
        hand_over(hop).wait_recv()

    for column in range(tp_count):
        block = contract_rows(full[:, column * width : (column + 1) * width], mixed)
        per = sp_count // tp_count
        parts_out[column * per : (column + 1) * per] = block.reshape(
            per, width // per, channels
        ).astype(bf16)

    def give_parts(step):
        to = lax.rem(me + step, sp_count)
        return remote(
            parts_out.at[to],
            parts_in.at[step],
            parts_send.at[step],
            parts_recv.at[step],
            sp=to,
        )

    for step in range(1, sp_count):
        begin(give_parts(step))

    grad_mixed = jnp.dot(full[...], proj_ref[...], preferred_element_type=f32)
    grad_normed = grad_mixed * norm_sigmoid * (1.0 + normed * (1.0 - norm_sigmoid))
    share(
        1,
        (
            jnp.sum(grad_normed, axis=1, keepdims=True),
            jnp.sum(grad_normed * normed, axis=1, keepdims=True),
        ),
    )
    first_sum, second_sum = shared(1)
    grad_conv = inv_std * (
        grad_normed - first_sum / conv_width - normed * (second_sum / conv_width)
    )
    padded[:tok_count] = grad_conv
    rim = rim_in.shape[0]
    rim_copy = remote(
        padded.at[pl.ds(0, rim)],
        rim_in,
        rim_send.at[0],
        rim_recv.at[0],
        sp=lax.rem(me + sp_count - 1, sp_count),
    )
    begin(rim_copy)
    gate_sig = jax.nn.sigmoid(gate_ref[...].astype(f32))
    rim_copy.wait_recv()
    padded[tok_count:] = jnp.where(me == sp_count - 1, 0.0, rim_in[...])
    grad_glu = jnp.zeros((tok_count, channels), f32)
    for offset in range(taps_ref.shape[0]):
        grad_glu += taps_ref[offset : offset + 1] * padded[offset : offset + tok_count]
    grad_value_ref[...] = (grad_glu * gate_sig).astype(bf16)
    grad_gate_ref[...] = (
        grad_glu * value_ref[...].astype(f32) * gate_sig * (1.0 - gate_sig)
    ).astype(bf16)

    summed = parts_out[me].astype(f32)
    for step in range(1, sp_count):
        give_parts(step).wait_recv()
        summed += parts_in[step].astype(f32)
    grad_proj_ref[...] = summed
    for copy in started:
        copy.wait_send()


def finish(sp_count, tp_count, partial_rows, picks, upstream_own, *conv_args):
    conv_saved, out_proj, conv_taps = conv_args[:3]
    blocks, capacity, model_width = partial_rows.shape
    tok_count, channels = conv_saved.shape
    width = model_width // tp_count
    chips = tp_count // 2
    rim = -(-(conv_taps.shape[0] - 1) // 8) * 8
    dma, vmem = pltpu.SemaphoreType.DMA, pltpu.VMEM
    f32, bf16 = jnp.float32, jnp.bfloat16
    proj_rows = model_width // sp_count
    shape = jax.ShapeDtypeStruct
    return pl.pallas_call(
        functools.partial(tail_kernel, sp_count, tp_count),
        out_shape=(
            shape((tok_count, width), bf16),
            shape((tok_count, channels), bf16),
            shape((tok_count, channels), bf16),
            shape((proj_rows, channels), f32),
        ),
        in_specs=[pl.BlockSpec(memory_space=vmem)] * 8,
        out_specs=[pl.BlockSpec(memory_space=vmem)] * 4,
        scratch_shapes=[
            vmem((sp_count, chips, capacity, width), bf16),
            vmem((sp_count, chips - 1, capacity, width), bf16),
            vmem((sp_count, chips - 1, capacity, width), bf16),
            vmem((sp_count, capacity, width), bf16),
            vmem((sp_count, capacity, width), bf16),
            vmem((tok_count, model_width), bf16),
            vmem((2, 8, 128), f32),
            vmem((2, tp_count, 8, 128), f32),
            vmem((sp_count, proj_rows, channels), bf16),
            vmem((sp_count, proj_rows, channels), bf16),
            vmem((rim, channels), f32),
            vmem((tok_count + rim, channels), f32),
            dma((sp_count, chips)),
            dma((sp_count, chips)),
            dma((sp_count, chips - 1)),
            dma((sp_count, chips - 1)),
            dma((sp_count,)),
            dma((sp_count,)),
            dma((2, chips)),
            dma((2, chips)),
            dma((2, tp_count)),
            dma((2, tp_count)),
            dma((sp_count,)),
            dma((sp_count,)),
            dma((1,)),
            dma((1,)),
        ],
        compiler_params=pltpu.CompilerParams(collective_id=1, has_side_effects=True),
        name="finish",
    )(partial_rows, picks, upstream_own, *conv_args)


def expert_backward(expert_rows, expert_cot, gate_weight, up_weight, down_weight):
    gate_pre = jnp.dot(expert_rows, gate_weight, preferred_element_type=jnp.float32)
    up_pre = jnp.dot(expert_rows, up_weight, preferred_element_type=jnp.float32)
    capped = jnp.minimum(gate_pre, clamp_limit)
    clipped = jnp.clip(up_pre, -clamp_limit, clamp_limit)
    gate_sigmoid = jax.nn.sigmoid(glu_alpha * capped)
    act = (capped * gate_sigmoid * (clipped + 1.0)).astype(jnp.bfloat16)
    grad_down = contract_rows(act, expert_cot)
    grad_act = times_transposed(expert_cot, down_weight)
    slope = gate_sigmoid + glu_alpha * capped * gate_sigmoid * (1.0 - gate_sigmoid)
    grad_gate_pre = jnp.where(
        gate_pre < clamp_limit, grad_act * (clipped + 1.0) * slope, 0.0
    ).astype(jnp.bfloat16)
    grad_up_pre = jnp.where(
        jnp.abs(up_pre) < clamp_limit, grad_act * capped * gate_sigmoid, 0.0
    ).astype(jnp.bfloat16)
    grad_gate = contract_rows(expert_rows, grad_gate_pre)
    grad_up = contract_rows(expert_rows, grad_up_pre)
    return (grad_gate, grad_up, grad_down, grad_gate_pre, grad_up_pre)


def on_device(
    upstream,
    stream,
    routes,
    route_weights,
    glu_value,
    glu_gate,
    conv_taps,
    conv_saved,
    out_proj,
    expert_gate,
    expert_up,
    expert_down,
):
    tok_count = upstream.shape[0]
    model_width = upstream.shape[1]
    expert_count = lax.axis_size("sp")
    capacity = 4 * tok_count // expert_count
    slice_width = model_width // lax.axis_size("tp")
    column_start = lax.axis_index("tp") * slice_width
    targets = pair_rows(routes, expert_count, capacity)
    picks, row_weights = select_pairs(targets, route_weights, expert_count * capacity)
    stream_part = lax.dynamic_slice_in_dim(stream, column_start, slice_width, 1)
    upstream_part = lax.dynamic_slice_in_dim(upstream, column_start, slice_width, 1)
    send_rows = jnp.dot(picks, stream_part, preferred_element_type=jnp.float32).astype(jnp.bfloat16)
    send_cot = (
        row_weights[:, None] * jnp.dot(picks, upstream_part, preferred_element_type=jnp.float32)
    ).astype(jnp.bfloat16)
    part_shape = (expert_count, capacity, slice_width)
    got_rows, got_cot = dispatch(
        send_rows.reshape(part_shape),
        send_cot.reshape(part_shape),
        expert_count,
        lax.axis_size("tp"),
    )
    expert_rows = got_rows.reshape(-1, model_width)
    expert_cot = got_cot.reshape(-1, model_width)
    gate_weight = expert_gate[0]
    up_weight = expert_up[0]
    down_weight = expert_down[0]
    grad_gate_w, grad_up_w, grad_down_w, grad_gate_pre, grad_up_pre = expert_backward(
        expert_rows, expert_cot, gate_weight, up_weight, down_weight
    )
    partial_rows = times_transposed(grad_gate_pre, gate_weight) + times_transposed(
        grad_up_pre, up_weight
    )
    grad_stream, grad_value, grad_gate, grad_out_proj = finish(
        expert_count,
        lax.axis_size("tp"),
        partial_rows.astype(jnp.bfloat16).reshape(expert_count, capacity, model_width),
        picks.T,
        upstream_part,
        conv_saved,
        out_proj,
        conv_taps,
        glu_value,
        glu_gate,
    )
    return (
        grad_stream,
        grad_value,
        grad_gate,
        grad_out_proj,
        grad_gate_w[None],
        grad_up_w[None],
        grad_down_w[None],
    )


def solution(mesh):
    in_specs = (
        P("sp", None),
        P("sp", None),
        P("sp", None),
        P("sp", None),
        P("sp", "tp"),
        P("sp", "tp"),
        P(None, "tp"),
        P("sp", "tp"),
        P(None, "tp"),
        P("sp", None, "tp"),
        P("sp", None, "tp"),
        P("sp", "tp", None),
    )
    out_specs = (
        P("sp", "tp"),
        P("sp", "tp"),
        P("sp", "tp"),
        P("sp", "tp"),
        P("sp", None, "tp"),
        P("sp", None, "tp"),
        P("sp", "tp", None),
    )
    return jax.shard_map(
        on_device, mesh=mesh, in_specs=in_specs, out_specs=out_specs, check_vma=False
    )
```

```python
import functools

import jax
import jax.numpy as jnp
from jax import lax
from jax.experimental import pallas as pl
from jax.experimental.pallas import tpu as pltpu
from jax.sharding import PartitionSpec as P


clamp_limit = 7.0
glu_alpha = 1.702
norm_eps = 1e-05


def contract_rows(left, right):
    return lax.dot_general(
        left, right, (((0,), (0,)), ((), ())), preferred_element_type=jnp.float32
    )


def times_transposed(left, right):
    return lax.dot_general(
        left, right, (((1,), (1,)), ((), ())), preferred_element_type=jnp.float32
    )


def pair_rows(block_routes, expert_count, capacity):
    tok_count, topk = block_routes.shape
    experts = jnp.arange(expert_count, dtype=jnp.int32)[None, :]
    hots = [(block_routes[:, k : k + 1] == experts).astype(jnp.float32) for k in range(topk)]
    before = (
        jnp.arange(tok_count)[:, None] > jnp.arange(tok_count)[None, :]
    ).astype(jnp.bfloat16)
    earlier = jnp.dot(before, sum(hots).astype(jnp.bfloat16), preferred_element_type=jnp.float32)
    slots = [jnp.sum(earlier * hot, axis=1).astype(jnp.int32) for hot in hots]
    return [block_routes[:, k] * capacity + slots[k] for k in range(topk)]


def select_pairs(targets, block_weights, row_count):
    rows = jnp.arange(row_count, dtype=jnp.int32)[:, None]
    hits = [target[None, :] == rows for target in targets]
    picks = sum(hit.astype(jnp.float32) for hit in hits).astype(jnp.bfloat16)
    row_weights = jnp.sum(
        sum(jnp.where(hit, block_weights[:, k][None, :], 0.0) for k, hit in enumerate(hits)), axis=1
    )
    return picks, row_weights


def greet(sp_count, tp_count):
    me, lane = lax.axis_index("sp"), lax.axis_index("tp")
    barrier = pltpu.get_barrier_semaphore()
    for step in range(1, sp_count):
        pl.semaphore_signal(
            barrier,
            inc=1,
            device_id={"sp": lax.rem(me + step, sp_count)},
            device_id_type=pl.DeviceIdType.MESH,
        )
    for step in range(1, tp_count):
        pl.semaphore_signal(
            barrier,
            inc=1,
            device_id={"tp": lax.rem(lane + step, tp_count)},
            device_id_type=pl.DeviceIdType.MESH,
        )
    pl.semaphore_wait(barrier, sp_count + tp_count - 2)


def remote(src, dst, send_sem, recv_sem, **target):
    return pltpu.make_async_remote_copy(
        src_ref=src,
        dst_ref=dst,
        send_sem=send_sem,
        recv_sem=recv_sem,
        device_id=target,
        device_id_type=pl.DeviceIdType.MESH,
    )


def dispatch_kernel(
    sp_count,
    tp_count,
    rows_ref,
    cot_ref,
    own_rows_ref,
    own_cot_ref,
    got_rows,
    got_cot,
    far_send,
    far_recv,
    side_send,
    side_recv,
    pair_send,
    pair_recv,
    own_sem,
):
    me, lane = lax.axis_index("sp"), lax.axis_index("tp")
    width = rows_ref.shape[2]
    chips = tp_count // 2
    partner = lane + 1 - 2 * lax.rem(lane, 2)
    sources, results = (rows_ref, cot_ref), (got_rows, got_cot)

    def place(which, block, column):
        return results[which].at[block, :, pl.ds(pl.multiple_of(column * width, width), width)]

    greet(sp_count, tp_count)

    def far(which, step):
        to = lax.rem(me + step, sp_count)
        return remote(
            sources[which].at[to],
            place(which, me, lane),
            far_send.at[which, step],
            far_recv.at[which, step],
            sp=to,
        )

    def beside(which, step, hop):
        block = lax.rem(me + sp_count - step, sp_count)
        return remote(
            place(which, block, lane),
            place(which, block, lane),
            side_send.at[which, step, hop],
            side_recv.at[which, step, hop],
            tp=lax.rem(lane + 2 * hop, tp_count),
        )

    def paired(which, step, hop):
        block = lax.rem(me + sp_count - step, sp_count)
        column = lax.rem(lane + tp_count - 2 * hop, tp_count)
        return remote(
            place(which, block, column),
            place(which, block, column),
            pair_send.at[which, step, hop],
            pair_recv.at[which, step, hop],
            tp=partner,
        )

    started = []

    def begin(copy):
        copy.start()
        started.append(copy)

    own = [
        pltpu.make_async_copy(own_rows_ref, got_rows.at[me], own_sem.at[0]),
        pltpu.make_async_copy(own_cot_ref, got_cot.at[me], own_sem.at[1]),
    ]
    for which in range(2):
        own[which].start()
        for step in range(1, sp_count):
            begin(far(which, step))
    arrivals = []
    for which in range(2):
        arrivals += [(which, step) for step in range(1, sp_count)]
    lag = 2
    for at in range(len(arrivals) + lag):
        if at < len(arrivals):
            which, step = arrivals[at]
            far(which, step).wait_recv()
            for hop in range(1, chips):
                begin(beside(which, step, hop))
            begin(paired(which, step, 0))
        if at >= lag:
            which, step = arrivals[at - lag]
            for hop in range(1, chips):
                beside(which, step, hop).wait_recv()
                begin(paired(which, step, hop))
    for which, step in arrivals:
        for hop in range(chips):
            paired(which, step, hop).wait_recv()
    for copy in started:
        copy.wait_send()
    for copy in own:
        copy.wait()


def dispatch(send_rows, send_cot, own_rows, own_cot, sp_count, tp_count):
    blocks, capacity, width = send_rows.shape
    full = jax.ShapeDtypeStruct((blocks, capacity, width * tp_count), send_rows.dtype)
    dma = pltpu.SemaphoreType.DMA
    chips = tp_count // 2
    return pl.pallas_call(
        functools.partial(dispatch_kernel, sp_count, tp_count),
        out_shape=(full, full),
        in_specs=[pl.BlockSpec(memory_space=pltpu.VMEM)] * 4,
        out_specs=[pl.BlockSpec(memory_space=pl.ANY)] * 2,
        scratch_shapes=[dma((2, sp_count))] * 2
        + [dma((2, sp_count, chips))] * 4
        + [dma((2,))],
        compiler_params=pltpu.CompilerParams(collective_id=0, has_side_effects=True),
        name="dispatch",
    )(send_rows, send_cot, own_rows, own_cot)


def tail_kernel(
    sp_count,
    tp_count,
    partial_ref,
    picks_ref,
    upstream_ref,
    saved_ref,
    proj_ref,
    taps_ref,
    value_ref,
    gate_ref,
    grad_stream_ref,
    grad_value_ref,
    grad_gate_ref,
    grad_proj_ref,
    pair_in,
    side_out,
    side_in,
    total,
    returned,
    full,
    stat_out,
    stat_in,
    parts_out,
    parts_in,
    rim_in,
    padded,
    pair_send,
    pair_recv,
    side_send,
    side_recv,
    far_send,
    far_recv,
    full_send,
    full_recv,
    stat_send,
    stat_recv,
    parts_send,
    parts_recv,
    rim_send,
    rim_recv,
):
    me, lane = lax.axis_index("sp"), lax.axis_index("tp")
    width = returned.shape[2]
    chips = tp_count // 2
    core = lax.rem(lane, 2)
    partner = lane + 1 - 2 * core
    tok_count, channels = saved_ref.shape
    conv_width = channels * tp_count
    groups = tok_count // 128
    f32, bf16 = jnp.float32, jnp.bfloat16

    greet(sp_count, tp_count)
    started = []

    def begin(copy):
        copy.start()
        started.append(copy)

    def columns(column):
        return pl.ds(pl.multiple_of(column * width, width), width)

    def swapped(step, hop):
        block = lax.rem(me + step, sp_count)
        other = lax.rem(lane + 2 * hop, tp_count) + 1 - 2 * core
        return remote(
            partial_ref.at[block, :, columns(other)],
            pair_in.at[step, hop],
            pair_send.at[step, hop],
            pair_recv.at[step, hop],
            tp=partner,
        )

    def beside(step, hop):
        return remote(
            side_out.at[step, hop - 1],
            side_in.at[step, hop - 1],
            side_send.at[step, hop - 1],
            side_recv.at[step, hop - 1],
            tp=lax.rem(lane + 2 * hop, tp_count),
        )

    def far(step):
        return remote(
            total.at[step],
            returned.at[me],
            far_send.at[step],
            far_recv.at[step],
            sp=lax.rem(me + step, sp_count),
        )

    order = list(range(1, sp_count)) + [0]
    for step in order:
        for hop in list(range(1, chips)) + [0]:
            begin(swapped(step, hop))

    eye = (
        lax.broadcasted_iota(jnp.int32, (128, 128), 0)
        == lax.broadcasted_iota(jnp.int32, (128, 128), 1)
    )

    def stat(phase, hop):
        return remote(
            stat_out.at[phase],
            stat_in.at[phase, hop],
            stat_send.at[phase, hop],
            stat_recv.at[phase, hop],
            tp=lax.rem(lane + hop, tp_count),
        )

    def share(phase, sums):
        stat_out[phase] = jnp.zeros(stat_out.shape[1:], f32)
        row = 0
        for item in sums:
            for group in range(groups):
                part = item[group * 128 : (group + 1) * 128]
                spread = jnp.where(eye, jnp.broadcast_to(part, (128, 128)), 0.0)
                stat_out[phase, row : row + 1] = jnp.sum(spread, axis=0, keepdims=True)
                row += 1
        for hop in range(1, tp_count):
            begin(stat(phase, hop))

    def shared(phase):
        value = stat_out[phase]
        for hop in range(1, tp_count):
            stat(phase, hop).wait_recv()
            value += stat_in[phase, hop]
        columns_of = []
        for item in range(2):
            parts = []
            for group in range(groups):
                row = item * groups + group
                spread = jnp.broadcast_to(value[row : row + 1], (128, 128))
                parts.append(jnp.sum(jnp.where(eye, spread, 0.0), axis=1, keepdims=True))
            columns_of.append(jnp.concatenate(parts, axis=0))
        return columns_of

    saved_conv = saved_ref[...].astype(f32)
    share(
        0,
        (
            jnp.sum(saved_conv, axis=1, keepdims=True),
            jnp.sum(saved_conv * saved_conv, axis=1, keepdims=True),
        ),
    )

    def pair_sum(step, hop):
        block = lax.rem(me + step, sp_count)
        column = lax.rem(lane + 2 * hop, tp_count)
        return partial_ref[block, :, columns(column)].astype(f32) + pair_in[step, hop].astype(f32)

    lag = 2
    for at in range(sp_count + lag):
        if at < sp_count:
            step = order[at]
            for hop in range(1, chips):
                swapped(step, hop).wait_recv()
                side_out[step, hop - 1] = pair_sum(step, hop).astype(bf16)
                begin(beside(step, hop))
        if at >= lag:
            step = order[at - lag]
            swapped(step, 0).wait_recv()
            value = pair_sum(step, 0)
            for hop in range(1, chips):
                beside(step, hop).wait_recv()
                value += side_in[step, hop - 1].astype(f32)
            if step:
                total[step] = value.astype(bf16)
                begin(far(step))
            else:
                returned[me] = value.astype(bf16)

    total_sum, square_sum = shared(0)
    mean_c = total_sum / conv_width
    var_c = square_sum / conv_width - mean_c * mean_c
    inv_std = lax.rsqrt(var_c + norm_eps)
    normed = (saved_conv - mean_c) * inv_std
    norm_sigmoid = jax.nn.sigmoid(normed)
    mixed = (normed * norm_sigmoid).astype(bf16)

    for step in range(1, sp_count):
        far(step).wait_recv()
    routed_sum = jnp.dot(
        picks_ref[...],
        returned[...].reshape(-1, width),
        preferred_element_type=f32,
    )
    own_grad = (upstream_ref[...].astype(f32) + routed_sum).astype(bf16)
    grad_stream_ref[...] = own_grad
    full[:, columns(lane)] = own_grad

    def spread_full(hop):
        return remote(
            full.at[:, columns(lane)],
            full.at[:, columns(lane)],
            full_send.at[0, hop],
            full_recv.at[0, hop],
            tp=lax.rem(lane + 2 * hop, tp_count),
        )

    def hand_over(hop):
        column = lax.rem(lane + tp_count - 2 * hop, tp_count)
        return remote(
            full.at[:, columns(column)],
            full.at[:, columns(column)],
            full_send.at[1, hop],
            full_recv.at[1, hop],
            tp=partner,
        )

    for hop in range(1, chips):
        begin(spread_full(hop))
    begin(hand_over(0))
    for hop in range(1, chips):
        spread_full(hop).wait_recv()
        begin(hand_over(hop))
    for hop in range(chips):
        hand_over(hop).wait_recv()

    for column in range(tp_count):
        block = contract_rows(full[:, column * width : (column + 1) * width], mixed)
        per = sp_count // tp_count
        parts_out[column * per : (column + 1) * per] = block.reshape(
            per, width // per, channels
        ).astype(bf16)

    def give_parts(step):
        to = lax.rem(me + step, sp_count)
        return remote(
            parts_out.at[to],
            parts_in.at[step],
            parts_send.at[step],
            parts_recv.at[step],
            sp=to,
        )

    for step in range(1, sp_count):
        begin(give_parts(step))

    grad_mixed = jnp.dot(full[...], proj_ref[...], preferred_element_type=f32)
    grad_normed = grad_mixed * norm_sigmoid * (1.0 + normed * (1.0 - norm_sigmoid))
    share(
        1,
        (
            jnp.sum(grad_normed, axis=1, keepdims=True),
            jnp.sum(grad_normed * normed, axis=1, keepdims=True),
        ),
    )
    first_sum, second_sum = shared(1)
    grad_conv = inv_std * (
        grad_normed - first_sum / conv_width - normed * (second_sum / conv_width)
    )
    padded[:tok_count] = grad_conv
    rim = rim_in.shape[0]
    rim_copy = remote(
        padded.at[pl.ds(0, rim)],
        rim_in,
        rim_send.at[0],
        rim_recv.at[0],
        sp=lax.rem(me + sp_count - 1, sp_count),
    )
    begin(rim_copy)
    gate_sig = jax.nn.sigmoid(gate_ref[...].astype(f32))
    rim_copy.wait_recv()
    padded[tok_count:] = jnp.where(me == sp_count - 1, 0.0, rim_in[...])
    grad_glu = jnp.zeros((tok_count, channels), f32)
    for offset in range(taps_ref.shape[0]):
        grad_glu += taps_ref[offset : offset + 1] * padded[offset : offset + tok_count]
    grad_value_ref[...] = (grad_glu * gate_sig).astype(bf16)
    grad_gate_ref[...] = (
        grad_glu * value_ref[...].astype(f32) * gate_sig * (1.0 - gate_sig)
    ).astype(bf16)

    summed = parts_out[me].astype(f32)
    for step in range(1, sp_count):
        give_parts(step).wait_recv()
        summed += parts_in[step].astype(f32)
    grad_proj_ref[...] = summed
    for copy in started:
        copy.wait_send()


def finish(sp_count, tp_count, partial_rows, picks, upstream_own, *conv_args):
    conv_saved, out_proj, conv_taps = conv_args[:3]
    blocks, capacity, model_width = partial_rows.shape
    tok_count, channels = conv_saved.shape
    width = model_width // tp_count
    chips = tp_count // 2
    rim = -(-(conv_taps.shape[0] - 1) // 8) * 8
    dma, vmem = pltpu.SemaphoreType.DMA, pltpu.VMEM
    f32, bf16 = jnp.float32, jnp.bfloat16
    proj_rows = model_width // sp_count
    shape = jax.ShapeDtypeStruct
    return pl.pallas_call(
        functools.partial(tail_kernel, sp_count, tp_count),
        out_shape=(
            shape((tok_count, width), bf16),
            shape((tok_count, channels), bf16),
            shape((tok_count, channels), bf16),
            shape((proj_rows, channels), f32),
        ),
        in_specs=[pl.BlockSpec(memory_space=vmem)] * 8,
        out_specs=[pl.BlockSpec(memory_space=vmem)] * 4,
        scratch_shapes=[
            vmem((sp_count, chips, capacity, width), bf16),
            vmem((sp_count, chips - 1, capacity, width), bf16),
            vmem((sp_count, chips - 1, capacity, width), bf16),
            vmem((sp_count, capacity, width), bf16),
            vmem((sp_count, capacity, width), bf16),
            vmem((tok_count, model_width), bf16),
            vmem((2, 8, 128), f32),
            vmem((2, tp_count, 8, 128), f32),
            vmem((sp_count, proj_rows, channels), bf16),
            vmem((sp_count, proj_rows, channels), bf16),
            vmem((rim, channels), f32),
            vmem((tok_count + rim, channels), f32),
            dma((sp_count, chips)),
            dma((sp_count, chips)),
            dma((sp_count, chips - 1)),
            dma((sp_count, chips - 1)),
            dma((sp_count,)),
            dma((sp_count,)),
            dma((2, chips)),
            dma((2, chips)),
            dma((2, tp_count)),
            dma((2, tp_count)),
            dma((sp_count,)),
            dma((sp_count,)),
            dma((1,)),
            dma((1,)),
        ],
        compiler_params=pltpu.CompilerParams(collective_id=1, has_side_effects=True),
        name="finish",
    )(partial_rows, picks, upstream_own, *conv_args)


def expert_backward(expert_rows, expert_cot, gate_weight, up_weight, down_weight):
    gate_pre = jnp.dot(expert_rows, gate_weight, preferred_element_type=jnp.float32)
    up_pre = jnp.dot(expert_rows, up_weight, preferred_element_type=jnp.float32)
    capped = jnp.minimum(gate_pre, clamp_limit)
    clipped = jnp.clip(up_pre, -clamp_limit, clamp_limit)
    gate_sigmoid = jax.nn.sigmoid(glu_alpha * capped)
    act = (capped * gate_sigmoid * (clipped + 1.0)).astype(jnp.bfloat16)
    grad_down = contract_rows(act, expert_cot)
    grad_act = times_transposed(expert_cot, down_weight)
    slope = gate_sigmoid + glu_alpha * capped * gate_sigmoid * (1.0 - gate_sigmoid)
    grad_gate_pre = jnp.where(
        gate_pre < clamp_limit, grad_act * (clipped + 1.0) * slope, 0.0
    ).astype(jnp.bfloat16)
    grad_up_pre = jnp.where(
        jnp.abs(up_pre) < clamp_limit, grad_act * capped * gate_sigmoid, 0.0
    ).astype(jnp.bfloat16)
    grad_gate = contract_rows(expert_rows, grad_gate_pre)
    grad_up = contract_rows(expert_rows, grad_up_pre)
    return (grad_gate, grad_up, grad_down, grad_gate_pre, grad_up_pre)


def on_device(
    upstream,
    stream,
    routes,
    route_weights,
    glu_value,
    glu_gate,
    conv_taps,
    conv_saved,
    out_proj,
    expert_gate,
    expert_up,
    expert_down,
):
    tok_count = upstream.shape[0]
    model_width = upstream.shape[1]
    expert_count = lax.axis_size("sp")
    capacity = 4 * tok_count // expert_count
    slice_width = model_width // lax.axis_size("tp")
    column_start = lax.axis_index("tp") * slice_width
    targets = pair_rows(routes, expert_count, capacity)
    picks, row_weights = select_pairs(targets, route_weights, expert_count * capacity)
    stream_part = lax.dynamic_slice_in_dim(stream, column_start, slice_width, 1)
    upstream_part = lax.dynamic_slice_in_dim(upstream, column_start, slice_width, 1)
    send_rows = jnp.dot(picks, stream_part, preferred_element_type=jnp.float32).astype(jnp.bfloat16)
    send_cot = (
        row_weights[:, None] * jnp.dot(picks, upstream_part, preferred_element_type=jnp.float32)
    ).astype(jnp.bfloat16)
    own_start = lax.axis_index("sp") * capacity
    own_picks = lax.dynamic_slice_in_dim(picks, own_start, capacity, 0)
    own_weights = lax.dynamic_slice_in_dim(row_weights, own_start, capacity, 0)
    own_rows = jnp.dot(own_picks, stream, preferred_element_type=jnp.float32).astype(jnp.bfloat16)
    own_cot = (
        own_weights[:, None] * jnp.dot(own_picks, upstream, preferred_element_type=jnp.float32)
    ).astype(jnp.bfloat16)
    part_shape = (expert_count, capacity, slice_width)
    got_rows, got_cot = dispatch(
        send_rows.reshape(part_shape),
        send_cot.reshape(part_shape),
        own_rows,
        own_cot,
        expert_count,
        lax.axis_size("tp"),
    )
    expert_rows = got_rows.reshape(-1, model_width)
    expert_cot = got_cot.reshape(-1, model_width)
    gate_weight = expert_gate[0]
    up_weight = expert_up[0]
    down_weight = expert_down[0]
    grad_gate_w, grad_up_w, grad_down_w, grad_gate_pre, grad_up_pre = expert_backward(
        expert_rows, expert_cot, gate_weight, up_weight, down_weight
    )
    partial_rows = times_transposed(grad_gate_pre, gate_weight) + times_transposed(
        grad_up_pre, up_weight
    )
    grad_stream, grad_value, grad_gate, grad_out_proj = finish(
        expert_count,
        lax.axis_size("tp"),
        partial_rows.astype(jnp.bfloat16).reshape(expert_count, capacity, model_width),
        picks.T,
        upstream_part,
        conv_saved,
        out_proj,
        conv_taps,
        glu_value,
        glu_gate,
    )
    return (
        grad_stream,
        grad_value,
        grad_gate,
        grad_out_proj,
        grad_gate_w[None],
        grad_up_w[None],
        grad_down_w[None],
    )


def solution(mesh):
    in_specs = (
        P("sp", None),
        P("sp", None),
        P("sp", None),
        P("sp", None),
        P("sp", "tp"),
        P("sp", "tp"),
        P(None, "tp"),
        P("sp", "tp"),
        P(None, "tp"),
        P("sp", None, "tp"),
        P("sp", None, "tp"),
        P("sp", "tp", None),
    )
    out_specs = (
        P("sp", "tp"),
        P("sp", "tp"),
        P("sp", "tp"),
        P("sp", "tp"),
        P("sp", None, "tp"),
        P("sp", None, "tp"),
        P("sp", "tp", None),
    )
    return jax.shard_map(
        on_device, mesh=mesh, in_specs=in_specs, out_specs=out_specs, check_vma=False
    )
```
